32 devices in a mesh: tp: 32 (over z, y, x, core).
Axes of the slice: x: 2, y: 2, z: 4, core: 2. Of those that a mesh axis runs over, the one named last changes fastest.
Arguments:
- tokens: bfloat16 [4096, 256], P('tp'), may hold values from -20 to 20, as said below
- positions: int32 [256], replicated, may hold values from 1 to 3072, 262144 in all
- norm_gain: float32 [4096], replicated, may hold values from 0.1 to 1.9
- w_query: bfloat16 [1024, 4096], P('tp'), may hold values from -0.09375 to 0.09375
- w_key: bfloat16 [1024, 4096], P('tp'), may hold values from -0.09375 to 0.09375
- w_value: bfloat16 [2048, 4096], P('tp'), may hold values from -0.09375 to 0.09375
- w_outgate: bfloat16 [2048, 4096], P('tp'), may hold values from -0.09375 to 0.09375
- w_input: bfloat16 [4, 4096], replicated, may hold values from -0.09375 to 0.09375
- w_forget: bfloat16 [4, 4096], replicated, may hold values from -0.09375 to 0.09375
- bias_input: float32 [4], replicated, may hold values from -3 to 3
- bias_forget: float32 [4], replicated, may hold values from -1 to 4
- w_read: bfloat16 [4096, 2048], P('tp'), may hold values from -0.125 to 0.125
- cells: float32 [2048, 256, 256], P('tp'), may hold values from -4 to 4
- norms: float32 [1024, 256], replicated, may hold values from 0 to 0.5
- maxima: float32 [4, 256], replicated, may hold values from -1 to 1
Outputs:
- mixed_rows: bfloat16 [4096, 256], P('tp')
- new_cells: float32 [2048, 256, 256], P('tp')
- new_norms: float32 [1024, 256], replicated
- new_maxima: float32 [4, 256], replicated
The draws below stay inside these ranges and needn't reach their ends.
Inputs may be any that keep to these rules, and one draw needn't show every extreme that they name: `tokens`: feature rows have their own scales, spread over a factor of ten.
All inputs are finite; a program needn't handle non-finite values.
Results may differ from the reference program's by a relative error of at most 0.0062.
The reference program's roundings to bfloat16 on the way (of `normed`, `query`, `key` and `gated`) count: a program that leaves them out, or rounds other values in their place, can miss the bound.
Values may be sent and summed in bfloat16 or wider, within the bound.
A program may use at most 128 MiB of HBM per device.

```python
import math
import jax
import jax.numpy as jnp
import numpy as np
from jax import lax

D = 4096
HEADS = 4
DQK = 256
DV = 512
BATCH = 256
MEAN_LEN = 1024
MOST_LEN = 3072


def draw_tokens(key, part):
    first, second = jax.random.split(key)
    row_scale = jnp.exp(jax.random.uniform(second, (D, 1), jnp.float32, -1.2, 1.2))
    base = jnp.clip(jax.random.normal(first, (D, BATCH), jnp.float32), -6.0, 6.0)
    return (base * row_scale).astype(jnp.bfloat16)


def level_of(key, dims, cuts, least, largest):
    factor_of = 1.0
    for axis_at, shards_of in cuts:
        draws = jax.random.uniform(jax.random.fold_in(jax.random.fold_in(key, 6), axis_at), (shards_of,), jnp.float32, least / len(cuts), largest / len(cuts))
        factor_of = factor_of * jnp.repeat(jnp.exp(draws), dims[axis_at] // shards_of).reshape((-1,) + (1,) * (len(dims) - 1 - axis_at))
    return factor_of


def length_profile(number_of, total, reach, slope):
    loads = [(1 << 20) // math.isqrt(rank ** slope) + 1 for rank in range(2, number_of + 1)]
    rest, counts = total - reach - (number_of - 1), [1] * (number_of - 1)
    while rest > 0:
        candidates = [i for i in range(number_of - 1) if counts[i] < reach]
        whole, remaining = sum([loads[i] for i in candidates]), rest
        for i in candidates:
            addition = min(reach - counts[i], max(1, remaining * loads[i] // whole), rest)
            counts[i] = counts[i] + addition
            rest = rest - addition
    return np.array([reach] + counts)


def ragged(stream_key, count, total, limit, lean):
    if count == 2:
        one = jax.random.randint(stream_key, (), max(1, total - limit), min(limit, total - 1) + 1)
        return jnp.stack([one, total - one])
    tallies = jnp.asarray(length_profile(count, total, limit, lean), jnp.int32)
    couples = (count - 1) // 2
    donor, taker = tallies[1:1 + 2 * couples:2], tallies[2:2 + 2 * couples:2]
    margin = jnp.minimum(donor - 1, limit - taker)
    moved = jax.random.randint(jax.random.fold_in(stream_key, 1), (couples,), 0, 1 << 20) % (margin + 1)
    tallies = tallies.at[1:1 + 2 * couples:2].set(donor - moved).at[2:2 + 2 * couples:2].set(taker + moved)
    return tallies[jax.random.permutation(jax.random.fold_in(stream_key, 2), count)]


def bell_draw(stream_key, dims, scale, most, cuts=(), kind=jnp.bfloat16):
    level = level_of(stream_key, dims, cuts, -0.22, 0.18) if cuts else 1.0
    drawn = jax.random.normal(stream_key, dims, jnp.float32) * scale * level
    return jnp.minimum(jnp.maximum(drawn, -most), most).astype(kind)


def setup_inputs(seed: int = 0) -> dict:
    arg_keys = jax.random.split(jax.random.key(seed), 16)
    tokens = draw_tokens(jax.random.fold_in(arg_keys[15], 71), 0)
    positions = ragged(arg_keys[1], BATCH, BATCH * MEAN_LEN, MOST_LEN, 2).astype(jnp.int32)
    norm_gain = jnp.clip(1.0 + 0.18 * jax.random.normal(arg_keys[2], (D,), jnp.float32), 0.1, 1.9)
    w_query = bell_draw(arg_keys[3], (HEADS * DQK, D), D ** -0.5, 0.09375, ((0, 32),))
    w_key = bell_draw(arg_keys[4], (HEADS * DQK, D), D ** -0.5, 0.09375, ((0, 32),))
    w_value = bell_draw(arg_keys[5], (HEADS * DV, D), D ** -0.5, 0.09375, ((0, 32),))
    w_outgate = bell_draw(arg_keys[6], (HEADS * DV, D), D ** -0.5, 0.09375, ((0, 32),))
    w_input = bell_draw(arg_keys[7], (HEADS, D), D ** -0.5, 0.09375)
    w_forget = bell_draw(arg_keys[8], (HEADS, D), D ** -0.5, 0.09375)
    bias_input = bell_draw(arg_keys[9], (HEADS,), 1.0, 3.0, (), jnp.float32)
    bias_forget = jnp.clip(jax.random.uniform(arg_keys[10], (HEADS,), jnp.float32, -1.0, 4.0), -1.0, 4.0)
    w_read = bell_draw(arg_keys[11], (D, HEADS * DV), (HEADS * DV) ** -0.5, 0.125, ((0, 32),))
    cells = bell_draw(arg_keys[12], (HEADS * DV, DQK, BATCH), 0.25, 4.0, ((0, 32),), jnp.float32)
    norms = jnp.clip(jax.random.uniform(arg_keys[13], (HEADS * DQK, BATCH), jnp.float32, 0.0, 0.5), 0.0, 0.5)
    maxima = jnp.clip(jax.random.uniform(arg_keys[14], (HEADS, BATCH), jnp.float32, -1.0, 1.0), -1.0, 1.0)
    return {"tokens": tokens, "positions": positions, "norm_gain": norm_gain, "w_query": w_query, "w_key": w_key, "w_value": w_value, "w_outgate": w_outgate, "w_input": w_input, "w_forget": w_forget, "bias_input": bias_input, "bias_forget": bias_forget, "w_read": w_read, "cells": cells, "norms": norms, "maxima": maxima}


EPS = 1e-06

def reference(tokens, positions, norm_gain, w_query, w_key, w_value, w_outgate, w_input, w_forget, bias_input, bias_forget, w_read, cells, norms, maxima):
    where = positions.astype(jnp.float32)[None, :]
    wide = tokens.astype(jnp.float32)
    total = lax.optimization_barrier(jnp.sum(wide * wide, axis=0))
    scale = lax.rsqrt(total / D + EPS)[None, :]
    normed = (wide * norm_gain[:, None]).astype(jnp.bfloat16)
    query = (jnp.dot(w_query, normed, preferred_element_type=jnp.float32) * scale).astype(jnp.bfloat16)
    key = (jnp.dot(w_key, normed, preferred_element_type=jnp.float32) * scale * DQK ** (-0.5)).astype(jnp.bfloat16)
    value = jnp.dot(w_value, normed, preferred_element_type=jnp.float32) * scale
    outgate = jnp.dot(w_outgate, normed, preferred_element_type=jnp.float32) * scale
    gate_in = jnp.dot(w_input, normed, preferred_element_type=jnp.float32) * scale + bias_input[:, None]
    gate_forget = jnp.dot(w_forget, normed, preferred_element_type=jnp.float32) * scale + bias_forget[:, None]
    logf = jax.nn.log_sigmoid(gate_forget) * (1.0 + where / MOST_LEN)
    new_max = jnp.maximum(logf + maxima, gate_in)
    decay = jnp.exp(logf + maxima - new_max)
    fresh = jnp.exp(gate_in - new_max)
    head_cells, head_norms, head_out = ([], [], [])
    for head in range(HEADS):
        q_head = query[head * DQK:(head + 1) * DQK].astype(jnp.float32)
        k_head = key[head * DQK:(head + 1) * DQK].astype(jnp.float32)
        v_head = value[head * DV:(head + 1) * DV]
        c_old = cells[head * DV:(head + 1) * DV]
        n_old = norms[head * DQK:(head + 1) * DQK]
        c_new = decay[head][None, None, :] * c_old + fresh[head][None, None, :] * v_head[:, None, :] * k_head[None, :, :]
        n_new = decay[head][None, :] * n_old + fresh[head][None, :] * k_head
        denom = lax.optimization_barrier(jnp.sum(q_head * n_new, axis=0))
        numer = lax.optimization_barrier(jnp.sum(q_head[None, :, :] * c_new, axis=1))
        head_out.append(numer / jnp.maximum(jnp.abs(denom), 1.0)[None, :])
        head_cells.append(c_new)
        head_norms.append(n_new)
    hidden = jnp.concatenate(head_out, axis=0)
    gated = (hidden * jax.nn.sigmoid(outgate)).astype(jnp.bfloat16)
    mixed = jnp.dot(w_read, gated, preferred_element_type=jnp.float32)
    rows = (wide + mixed).astype(jnp.bfloat16)
    return (rows, jnp.concatenate(head_cells, axis=0), jnp.concatenate(head_norms, axis=0), new_max)
```

```python
import functools

import jax
import jax.numpy as jnp
from jax import lax
from jax.experimental import pallas as pl
from jax.experimental.pallas import tpu as pltpu
from jax.sharding import PartitionSpec as P

DQK = 256
MOST_LEN = 3072


EPS = 1e-06

MESH = pl.DeviceIdType.MESH
ANY = pl.BlockSpec(memory_space=pl.ANY)
VM = pl.BlockSpec(memory_space=pltpu.VMEM)
SIDES = (0, 2, 4, 6)


def flip(me, mask):
    out, bit = me, 1
    while bit <= mask:
        if mask & bit:
            out = out + bit * (1 - 2 * ((me // bit) % 2))
        bit *= 2
    return out


def greet(me, masks):
    barrier = pltpu.get_barrier_semaphore()
    for mask in masks:
        pl.semaphore_signal(
            barrier, inc=1, device_id=(flip(me, mask),), device_id_type=MESH
        )
    pl.semaphore_wait(barrier, len(masks))


class Gather:
    def __init__(self, me, planes, src, buf, send, recv):
        self.me, self.planes, self.src, self.buf = me, planes, src, buf
        self.send, self.recv = send, recv
        self.rows = buf.shape[1]
        self.sent, self.number = [], 0

    def put(self, mask, origin_mask, slot, part=None):
        origin = flip(self.me, origin_mask)
        src = self.src if origin_mask == 0 else self.buf.at[origin]
        dst = self.buf.at[origin]
        if part is not None:
            half = self.rows // 2
            src = src.at[pl.ds(part * half, half)]
            dst = dst.at[pl.ds(part * half, half)]
        copy = pltpu.make_async_remote_copy(
            src_ref=src,
            dst_ref=dst,
            send_sem=self.send.at[self.number],
            recv_sem=self.recv.at[slot],
            device_id=(flip(self.me, mask),),
            device_id_type=MESH,
        )
        self.number += 1
        copy.start()
        self.sent.append(copy)

    def got(self, origin_mask, slot, part=None):
        dst = self.buf.at[flip(self.me, origin_mask)]
        if part is not None:
            half = self.rows // 2
            dst = dst.at[pl.ds(part * half, half)]
        pltpu.make_async_copy(dst, dst, self.recv.at[slot]).wait()

    def begin(self):
        for m in range(1, self.planes):
            self.put(8 * m, 0, 10 * m)
        self.put(2, 0, 1)
        self.put(4, 0, 2)
        self.put(1, 0, 5)

    def z(self, m):
        self.got(8 * m, 10 * m)
        self.put(2, 8 * m, 10 * m + 1)
        self.put(4, 8 * m, 10 * m + 2)
        self.put(1, 8 * m, 10 * m + 5)

    def x(self, m):
        self.got(8 * m + 2, 10 * m + 1)
        self.put(4, 8 * m + 2, 10 * m + 3, 0)
        self.put(1, 8 * m + 2, 10 * m + 6)

    def y(self, m):
        self.got(8 * m + 4, 10 * m + 2)
        self.put(2, 8 * m + 4, 10 * m + 4, 1)
        self.put(1, 8 * m + 4, 10 * m + 7)

    def d(self, m):
        for part in range(2):
            self.got(8 * m + 6, 10 * m + 3 + part, part)
            self.put(1, 8 * m + 6, 10 * m + 8 + part, part)

    def sibling(self, m, side):
        origin = 8 * m + SIDES[side] + 1
        if side == 3:
            for part in range(2):
                self.got(origin, 10 * m + 8 + part, part)
        else:
            self.got(origin, 10 * m + 5 + side)

    def end(self):
        for copy in self.sent:
            copy.wait_send()

    @staticmethod
    def sends(planes):
        return 10 * planes - 1

    def events(self):
        steps = []
        for m in range(self.planes + 2):
            if 1 <= m < self.planes:
                steps.append((self.z, m, 0))
            if 1 <= m <= self.planes:
                steps.append((self.x, m - 1, 1))
                steps.append((self.y, m - 1, 2))
            if 2 <= m:
                steps.append((self.d, m - 2, 3))
        return steps


def plane_masks(planes):
    return [1, 2, 4] + [8 * m for m in range(1, planes)]


def project_kernel(
    planes, width, most,
    tok, gain, w_q, w_k, w_v, w_o, w_i, w_f, b_i, b_f, where, maxima, cells,
    c_out, val_out, og_out, q_out, k_out, kown_out, max_out, dec_out, fre_out,
    buf, wbuf, gcol, acc, total, qk_own, qk_all,
    send, recv, qsend, qrecv, wsem, csem,
):
    me = lax.axis_index("tp")
    loads = []
    row = 0
    for number, ref in enumerate((w_q, w_k, w_v, w_o)):
        copy = pltpu.make_async_copy(
            ref, wbuf.at[pl.ds(row, ref.shape[0])], wsem.at[number]
        )
        copy.start()
        loads.append(copy)
        row += ref.shape[0]
    big = pltpu.make_async_copy(cells, c_out, csem)
    masks = plane_masks(planes) + [6]
    greet(me, masks)
    g = Gather(me, planes, tok, buf, send, recv)
    g.begin()
    big.start()
    buf[me] = tok[...]
    heads = w_i.shape[0]
    gates = jnp.concatenate(
        [w_i[...].astype(jnp.float32), w_f[...].astype(jnp.float32)], axis=0
    )
    wbuf[row : row + 16] = jnp.concatenate([gates, gates], axis=0).astype(jnp.bfloat16)
    rows = tok.shape[0]
    for part in range(width // 128):
        line = gain[part : part + 1, :]
        gcol[part * 128 : (part + 1) * 128] = jnp.transpose(
            jnp.broadcast_to(line, (128, 128))
        )
    acc[...] = jnp.zeros_like(acc)
    total[...] = jnp.zeros_like(total)
    for copy in loads:
        copy.wait()

    def take(m, side):
        g.sibling(m, side)
        chip = flip(me, 8 * m + SIDES[side]) // 2
        block = buf[pl.ds(chip * 2, 2)].astype(jnp.float32)
        block = block.reshape(2 * rows, block.shape[2])
        at = pl.multiple_of(chip * 2 * rows, 2 * rows)
        gains = gcol[pl.ds(at, 2 * rows), :]
        gains = jnp.concatenate([gains] * (block.shape[1] // 128), axis=1)
        normed = (block * gains).astype(jnp.bfloat16)
        squares = block * block
        total[...] += jnp.sum(squares.reshape(-1, 8, squares.shape[1]), axis=0)
        acc[...] += jnp.dot(
            wbuf[:, pl.ds(at, 2 * rows)], normed, preferred_element_type=jnp.float32
        )

    ready = [(0, 0)]
    for step, m, side in g.events():
        step(m)
        if ready:
            take(*ready.pop(0))
        ready.append((m, side))
    for item in ready:
        take(*item)

    scale = lax.rsqrt(jnp.sum(total[...], axis=0, keepdims=True) / width + EPS)
    nq = w_q.shape[0]
    nv = w_v.shape[0]
    q = (acc[0:nq] * scale).astype(jnp.bfloat16)
    k = (acc[nq : 2 * nq] * scale * DQK ** (-0.5)).astype(jnp.bfloat16)
    qk_own[0:nq] = q
    qk_own[nq : 2 * nq] = k
    mine = lax.rem(me, 8)
    copies = []

    def pass_on(mask, src, origin, slot):
        copy = pltpu.make_async_remote_copy(
            src_ref=src,
            dst_ref=qk_all.at[origin],
            send_sem=qsend.at[len(copies)],
            recv_sem=qrecv.at[slot],
            device_id=(flip(me, mask),),
            device_id_type=MESH,
        )
        copy.start()
        copies.append(copy)

    def arrived(origin, slot):
        ref = qk_all.at[origin]
        pltpu.make_async_copy(ref, ref, qrecv.at[slot]).wait()

    for mask in (6, 2, 4, 1):
        pass_on(mask, qk_own, mine, mask)
    qk_all[mine] = qk_own[...]
    kown_out[...] = k
    gate_in = acc[row : row + heads] * scale + b_i[...]
    gate_f = acc[row + heads : row + 2 * heads] * scale + b_f[...]
    soft = jnp.minimum(gate_f, 0.0) - jnp.log1p(jnp.exp(-jnp.abs(gate_f)))
    logf = soft * (1.0 + where[...].astype(jnp.float32) / most)
    lifted = logf + maxima[...]
    new_max = jnp.maximum(lifted, gate_in)
    max_out[...] = new_max
    dec_out[...] = jnp.exp(lifted - new_max)
    fre_out[...] = jnp.exp(gate_in - new_max)
    val_out[...] = acc[2 * nq : 2 * nq + nv] * scale
    og_out[...] = jax.nn.sigmoid(acc[2 * nq + nv : 2 * nq + 2 * nv] * scale)
    for mask in (2, 4, 6):
        origin = flip(mine, mask)
        arrived(origin, mask)
        pass_on(1, qk_all.at[origin], origin, mask + 1)
    for mask in (1, 3, 5, 7):
        arrived(flip(mine, mask), mask)
    for part in range(8):
        q_out[part * nq : (part + 1) * nq] = qk_all[part, 0:nq].astype(jnp.float32)
        k_out[part * nq : (part + 1) * nq] = qk_all[part, nq : 2 * nq].astype(jnp.float32)
    for copy in copies:
        copy.wait_send()
    g.end()
    big.wait()


GROUP = 4
SLOTS = 4


def cell_kernel(
    cells, val, og, q, k, dec, fre, norms,
    new_cells, gated,
    stage, numer, fv, nrm, den, sems, nsem,
):
    me = lax.axis_index("tp")
    head = me * dec.shape[0] // lax.axis_size("tp")
    dq = q.shape[0]
    load = pltpu.make_async_copy(norms.at[pl.ds(head * dq, dq)], nrm, nsem)
    load.start()
    decay = dec[pl.ds(head, 1), :]
    fresh = fre[pl.ds(head, 1), :]
    fv[...] = fresh * val[...]
    seqs = decay.shape[1]
    decay8 = jnp.broadcast_to(decay, (8, seqs))
    number = cells.shape[0] // GROUP

    def out_copy(step, slot):
        return pltpu.make_async_copy(
            stage.at[slot], new_cells.at[pl.ds(step * GROUP, GROUP)], sems.at[slot]
        )

    def body(step, carry):
        slot = lax.rem(step, SLOTS)

        @pl.when(step >= SLOTS)
        def _():
            out_copy(step - SLOTS, slot).wait()

        lines = [
            jnp.broadcast_to(fv[pl.ds(step * GROUP + i, 1), :], (8, seqs))
            for i in range(GROUP)
        ]
        sums = [jnp.zeros((8, seqs), jnp.float32)] * GROUP
        for d in range(0, dq, 8):
            qd, kd = q[d : d + 8], k[d : d + 8]
            for i in range(GROUP):
                new = decay8 * cells[step * GROUP + i, d : d + 8] + lines[i] * kd
                stage[slot, i, d : d + 8] = new
                sums[i] = sums[i] + qd * new
        for i in range(GROUP):
            numer[pl.ds(step * GROUP + i, 1), :] = jnp.sum(
                sums[i], axis=0, keepdims=True
            )
        out_copy(step, slot).start()
        return carry

    lax.fori_loop(0, number, body, 0)
    load.wait()
    denom = jnp.sum(q[...] * (decay * nrm[...] + fresh * k[...]), axis=0, keepdims=True)
    hidden = numer[...] / jnp.maximum(jnp.abs(denom), 1.0)
    gated[...] = (hidden * og[...]).astype(jnp.bfloat16)
    for step in range(number - SLOTS, number):
        out_copy(step, step % SLOTS).wait()


def read_kernel(
    planes, gated, kown, w_read, tok, mixed, keys, gbuf, wbuf,
    send, recv, ksend, krecv, wsem,
):
    me = lax.axis_index("tp")
    load = pltpu.make_async_copy(w_read, wbuf, wsem)
    load.start()
    greet(me, plane_masks(planes))
    g = Gather(me, planes, gated, gbuf, send, recv)
    h = Gather(me, planes, kown, keys, ksend, krecv)
    g.begin()
    h.begin()
    gbuf[me] = gated[...]
    keys[me] = kown[...]
    for (step, m, _), (other, _, _) in zip(g.events(), h.events()):
        step(m)
        other(m)
    for m in range(planes):
        for side in range(4):
            g.sibling(m, side)
    load.wait()
    whole = gbuf[...].reshape(-1, gbuf.shape[2])
    out = jnp.dot(wbuf[...], whole, preferred_element_type=jnp.float32)
    mixed[...] = (tok[...].astype(jnp.float32) + out).astype(jnp.bfloat16)
    for m in range(planes):
        for side in range(4):
            h.sibling(m, side)
    g.end()
    h.end()


def fused_block(
    rows, where, gain, w_query, w_key, w_value, w_outgate, w_input, w_forget,
    bias_input, bias_forget, w_read, cells, norms, maxima,
):
    count = lax.axis_size("tp")
    planes = count // 8
    width = gain.shape[0]
    heads = w_input.shape[0]
    seqs = rows.shape[1]
    nq, nv = w_query.shape[0], w_value.shape[0]
    f32, bf16 = jnp.float32, jnp.bfloat16
    total_w = 2 * nq + 2 * nv + 16
    sends = Gather.sends(planes)
    dma = pltpu.SemaphoreType.DMA
    c_vm, val, og, q, k, kown, new_max, dec, fre = pl.pallas_call(
        functools.partial(project_kernel, planes, width, MOST_LEN),
        out_shape=(
            pltpu.VMEM(cells.shape, f32),
            jax.ShapeDtypeStruct((nv, seqs), f32),
            jax.ShapeDtypeStruct((nv, seqs), f32),
            jax.ShapeDtypeStruct((8 * nq, seqs), f32),
            jax.ShapeDtypeStruct((8 * nq, seqs), f32),
            jax.ShapeDtypeStruct((nq, seqs), bf16),
            jax.ShapeDtypeStruct((heads, seqs), f32),
            jax.ShapeDtypeStruct((heads, seqs), f32),
            jax.ShapeDtypeStruct((heads, seqs), f32),
        ),
        in_specs=[VM, VM, ANY, ANY, ANY, ANY] + [VM] * 6 + [ANY],
        out_specs=[VM] * 9,
        scratch_shapes=[
            pltpu.VMEM((count, rows.shape[0], seqs), bf16),
            pltpu.VMEM((total_w, width), bf16),
            pltpu.VMEM((width, 128), f32),
            pltpu.VMEM((total_w, seqs), f32),
            pltpu.VMEM((8, seqs), f32),
            pltpu.VMEM((2 * nq, seqs), bf16),
            pltpu.VMEM((8, 2 * nq, seqs), bf16),
            dma((sends,)),
            dma((10 * planes,)),
            dma((7,)),
            dma((8,)),
            dma((4,)),
            dma,
        ],
        compiler_params=pltpu.CompilerParams(
            collective_id=0, has_side_effects=True, vmem_limit_bytes=K1_LIMIT
        ),
        name="project",
    )(
        rows, gain.reshape(width // 128, 128), w_query, w_key, w_value, w_outgate,
        w_input, w_forget, bias_input[:, None], bias_forget[:, None],
        where[None, :], maxima, cells,
    )
    new_cells, gated = pl.pallas_call(
        cell_kernel,
        out_shape=(
            jax.ShapeDtypeStruct(cells.shape, f32),
            jax.ShapeDtypeStruct((nv, seqs), bf16),
        ),
        in_specs=[VM] * 7 + [ANY],
        out_specs=[ANY, VM],
        scratch_shapes=[
            pltpu.VMEM((SLOTS, GROUP) + cells.shape[1:], f32),
            pltpu.VMEM((nv, seqs), f32),
            pltpu.VMEM((nv, seqs), f32),
            pltpu.VMEM((8 * nq, seqs), f32),
            pltpu.VMEM((8, seqs), f32),
            dma((SLOTS,)),
            dma,
        ],
        compiler_params=pltpu.CompilerParams(vmem_limit_bytes=K1_LIMIT),
        name="cells",
    )(c_vm, val, og, q, k, dec, fre, norms)
    mixed, keys = pl.pallas_call(
        functools.partial(read_kernel, planes),
        out_shape=(
            jax.ShapeDtypeStruct(rows.shape, bf16),
            jax.ShapeDtypeStruct((count, nq, seqs), bf16),
        ),
        in_specs=[VM, VM, ANY, VM],
        out_specs=[VM, VM],
        scratch_shapes=[
            pltpu.VMEM((count, nv, seqs), bf16),
            pltpu.VMEM(w_read.shape, bf16),
            dma((sends,)),
            dma((10 * planes,)),
            dma((sends,)),
            dma((10 * planes,)),
            dma,
        ],
        compiler_params=pltpu.CompilerParams(
            collective_id=1, has_side_effects=True, vmem_limit_bytes=K1_LIMIT
        ),
        name="readout",
    )(gated, kown, w_read, rows)
    keys = keys.astype(f32).reshape(heads, -1, seqs)
    norms_new = dec[:, None, :] * norms.reshape(keys.shape) + fre[:, None, :] * keys
    return mixed, new_cells, norms_new.reshape(norms.shape), new_max


K1_LIMIT = 30 * 1024 * 1024


def fits(count, rows, w_query, w_input, cells):
    planes = count // 8
    return (
        count % 8 == 0
        and planes & (planes - 1) == 0
        and w_input.shape[0] == planes
        and rows.shape[0] % 128 == 0
        and w_query.shape[0] % 32 == 0
        and cells.shape[0] % (GROUP * SLOTS) == 0
    )


def mix_block(
    rows,
    where,
    gain,
    w_query,
    w_key,
    w_value,
    w_outgate,
    w_input,
    w_forget,
    bias_input,
    bias_forget,
    w_read,
    cells,
    norms,
    maxima,
):
    count = lax.axis_size("tp")
    index = lax.axis_index("tp")
    seqs = rows.shape[1]
    model_width = gain.shape[0]
    heads = w_input.shape[0]
    head = index * heads // count
    whole = lax.all_gather(rows, "tp", axis=0, tiled=True).astype(jnp.float32)
    total = jnp.sum(whole * whole, axis=0)
    normed = (whole * gain[:, None]).astype(jnp.bfloat16)
    scale = lax.rsqrt(total / model_width + EPS)[None, :]
    query_loc = (jnp.dot(w_query, normed, preferred_element_type=jnp.float32) * scale).astype(
        jnp.bfloat16
    )
    key_loc = (
        jnp.dot(w_key, normed, preferred_element_type=jnp.float32) * scale * DQK ** (-0.5)
    ).astype(jnp.bfloat16)
    query_all, key_all = (
        lax.all_gather(query_loc, "tp", axis=0, tiled=True),
        lax.all_gather(key_loc, "tp", axis=0, tiled=True),
    )
    value = jnp.dot(w_value, normed, preferred_element_type=jnp.float32) * scale
    outgate = jnp.dot(w_outgate, normed, preferred_element_type=jnp.float32) * scale
    gate_in = (
        jnp.dot(w_input, normed, preferred_element_type=jnp.float32) * scale + bias_input[:, None]
    )
    gate_forget = (
        jnp.dot(w_forget, normed, preferred_element_type=jnp.float32) * scale + bias_forget[:, None]
    )
    logf = jax.nn.log_sigmoid(gate_forget) * (1.0 + where / MOST_LEN)
    new_max = jnp.maximum(logf + maxima, gate_in)
    decay = jnp.exp(logf + maxima - new_max)
    fresh = jnp.exp(gate_in - new_max)
    queries = query_all.astype(jnp.float32).reshape(heads, DQK, seqs)
    keys = key_all.astype(jnp.float32).reshape(heads, DQK, seqs)
    norms_new = decay[:, None, :] * norms.reshape(heads, DQK, seqs) + fresh[:, None, :] * keys
    denom = jnp.sum(queries * norms_new, axis=1)
    decay_own = lax.dynamic_index_in_dim(decay, head, 0)
    fresh_own = lax.dynamic_index_in_dim(fresh, head, 0)
    den_own = lax.dynamic_index_in_dim(denom, head, 0)
    q_head = lax.dynamic_slice_in_dim(query_all, head * DQK, DQK, 0).astype(jnp.float32)
    k_head = lax.dynamic_slice_in_dim(key_all, head * DQK, DQK, 0).astype(jnp.float32)
    new_cells = decay_own[None] * cells + fresh_own[None] * value[:, None, :] * k_head[None, :, :]
    numer = jnp.sum(q_head[None, :, :] * new_cells, axis=1)
    hidden = numer / jnp.maximum(jnp.abs(den_own), 1.0)
    gated = (hidden * jax.nn.sigmoid(outgate)).astype(jnp.bfloat16)
    mixed = jnp.dot(
        w_read, lax.all_gather(gated, "tp", axis=0, tiled=True), preferred_element_type=jnp.float32
    )
    new_rows = (rows.astype(jnp.float32) + mixed).astype(jnp.bfloat16)
    return (new_rows, new_cells, norms_new.reshape(heads * DQK, seqs), new_max)


def shards(
    tokens,
    positions,
    norm_gain,
    w_query,
    w_key,
    w_value,
    w_outgate,
    w_input,
    w_forget,
    bias_input,
    bias_forget,
    w_read,
    cells,
    norms,
    maxima,
):
    if fits(lax.axis_size("tp"), tokens, w_query, w_input, cells):
        block, where = fused_block, positions
    else:
        block, where = mix_block, positions.astype(jnp.float32)[None, :]
    return block(
        tokens,
        where,
        norm_gain,
        w_query,
        w_key,
        w_value,
        w_outgate,
        w_input,
        w_forget,
        bias_input,
        bias_forget,
        w_read,
        cells,
        norms,
        maxima,
    )


def solution(mesh):
    return jax.shard_map(
        shards,
        mesh=mesh,
        in_specs=(
            P("tp", None),
            P(),
            P(),
            P("tp", None),
            P("tp", None),
            P("tp", None),
            P("tp", None),
            P(),
            P(),
            P(),
            P(),
            P("tp", None),
            P("tp", None, None),
            P(),
            P(),
        ),
        out_specs=(P("tp", None), P("tp", None, None), P(), P()),
        check_vma=False,
    )
```

```python
import functools

import jax
import jax.numpy as jnp
from jax import lax
from jax.experimental import pallas as pl
from jax.experimental.pallas import tpu as pltpu
from jax.sharding import PartitionSpec as P

DQK = 256
MOST_LEN = 3072


EPS = 1e-06

MESH = pl.DeviceIdType.MESH
ANY = pl.BlockSpec(memory_space=pltpu.HBM)
VM = pl.BlockSpec(memory_space=pltpu.VMEM)
SIDES = (0, 2, 4, 6)


def flip(me, mask):
    out, bit = me, 1
    while bit <= mask:
        if mask & bit:
            out = out + bit * (1 - 2 * ((me // bit) % 2))
        bit *= 2
    return out


def greet(me, masks):
    barrier = pltpu.get_barrier_semaphore()
    for mask in masks:
        pl.semaphore_signal(
            barrier, inc=1, device_id=(flip(me, mask),), device_id_type=MESH
        )
    pl.semaphore_wait(barrier, len(masks))


class Gather:
    def __init__(self, me, planes, src, buf, send, recv):
        self.me, self.planes, self.src, self.buf = me, planes, src, buf
        self.send, self.recv = send, recv
        self.rows = buf.shape[1]
        self.sent, self.number = [], 0

    def put(self, mask, origin_mask, slot, part=None):
        origin = flip(self.me, origin_mask)
        src = self.src if origin_mask == 0 else self.buf.at[origin]
        dst = self.buf.at[origin]
        if part is not None:
            half = self.rows // 2
            src = src.at[pl.ds(part * half, half)]
            dst = dst.at[pl.ds(part * half, half)]
        copy = pltpu.make_async_remote_copy(
            src_ref=src,
            dst_ref=dst,
            send_sem=self.send.at[self.number],
            recv_sem=self.recv.at[slot],
            device_id=(flip(self.me, mask),),
            device_id_type=MESH,
        )
        self.number += 1
        copy.start()
        self.sent.append(copy)

    def got(self, origin_mask, slot, part=None):
        dst = self.buf.at[flip(self.me, origin_mask)]
        if part is not None:
            half = self.rows // 2
            dst = dst.at[pl.ds(part * half, half)]
        pltpu.make_async_copy(dst, dst, self.recv.at[slot]).wait()

    def begin(self):
        for m in range(1, self.planes):
            self.put(8 * m, 0, 10 * m)
        self.put(2, 0, 1)
        self.put(4, 0, 2)
        self.put(1, 0, 5)

    def z(self, m):
        self.got(8 * m, 10 * m)
        self.put(2, 8 * m, 10 * m + 1)
        self.put(4, 8 * m, 10 * m + 2)
        self.put(1, 8 * m, 10 * m + 5)

    def x(self, m):
        self.got(8 * m + 2, 10 * m + 1)
        self.put(4, 8 * m + 2, 10 * m + 3, 0)
        self.put(1, 8 * m + 2, 10 * m + 6)

    def y(self, m):
        self.got(8 * m + 4, 10 * m + 2)
        self.put(2, 8 * m + 4, 10 * m + 4, 1)
        self.put(1, 8 * m + 4, 10 * m + 7)

    def d(self, m):
        for part in range(2):
            self.got(8 * m + 6, 10 * m + 3 + part, part)
            self.put(1, 8 * m + 6, 10 * m + 8 + part, part)

    def sibling(self, m, side):
        origin = 8 * m + SIDES[side] + 1
        if side == 3:
            for part in range(2):
                self.got(origin, 10 * m + 8 + part, part)
        else:
            self.got(origin, 10 * m + 5 + side)

    def end(self):
        for copy in self.sent:
            copy.wait_send()

    @staticmethod
    def sends(planes):
        return 10 * planes - 1

    def events(self):
        steps = []
        for m in range(self.planes + 2):
            if 1 <= m < self.planes:
                steps.append((self.z, m, 0))
            if 1 <= m <= self.planes:
                steps.append((self.x, m - 1, 1))
                steps.append((self.y, m - 1, 2))
            if 2 <= m:
                steps.append((self.d, m - 2, 3))
        return steps


def plane_masks(planes):
    return [1, 2, 4] + [8 * m for m in range(1, planes)]


def project_kernel(
    planes, width, most,
    tok_in, gain_in, w_q, w_k, w_v, w_o, wi_in, wf_in, bi_in, bf_in, where_in,
    maxima_in, cells,
    c_out, val_out, og_out, q_out, k_out, kown_out, max_out, dec_out, fre_out,
    buf, wbuf, gcol, acc, total, qk_own, qk_all,
    tok, gain, w_i, w_f, b_i, b_f, where, maxima,
    send, recv, qsend, qrecv, wsem, csem, ssem,
):
    me = lax.axis_index("tp")
    small = []
    for number, (ref, here) in enumerate(
        (
            (tok_in, tok), (wi_in, w_i), (wf_in, w_f), (gain_in, gain),
            (bi_in, b_i), (bf_in, b_f), (where_in, where), (maxima_in, maxima),
        )
    ):
        copy = pltpu.make_async_copy(ref, here, ssem.at[number])
        copy.start()
        small.append(copy)
    loads = []
    row = 0
    for number, ref in enumerate((w_q, w_k, w_v, w_o)):
        copy = pltpu.make_async_copy(
            ref, wbuf.at[pl.ds(row, ref.shape[0])], wsem.at[number]
        )
        copy.start()
        loads.append(copy)
        row += ref.shape[0]
    big = pltpu.make_async_copy(cells, c_out, csem)
    masks = plane_masks(planes) + [6]
    greet(me, masks)
    g = Gather(me, planes, tok, buf, send, recv)
    small[0].wait()
    g.begin()
    big.start()
    for copy in small[1:]:
        copy.wait()
    buf[me] = tok[...]
    heads = w_i.shape[0]
    gates = jnp.concatenate(
        [w_i[...].astype(jnp.float32), w_f[...].astype(jnp.float32)], axis=0
    )
    wbuf[row : row + 16] = jnp.concatenate([gates, gates], axis=0).astype(jnp.bfloat16)
    rows = tok.shape[0]
    for part in range(width // 128):
        line = gain[part : part + 1, :]
        gcol[part * 128 : (part + 1) * 128] = jnp.transpose(
            jnp.broadcast_to(line, (128, 128))
        )
    acc[...] = jnp.zeros_like(acc)
    total[...] = jnp.zeros_like(total)
    for copy in loads:
        copy.wait()

    def take(m, side):
        g.sibling(m, side)
        chip = flip(me, 8 * m + SIDES[side]) // 2
        block = buf[pl.ds(chip * 2, 2)].astype(jnp.float32)
        block = block.reshape(2 * rows, block.shape[2])
        at = pl.multiple_of(chip * 2 * rows, 2 * rows)
        gains = gcol[pl.ds(at, 2 * rows), :]
        gains = jnp.concatenate([gains] * (block.shape[1] // 128), axis=1)
        normed = (block * gains).astype(jnp.bfloat16)
        squares = block * block
        total[...] += jnp.sum(squares.reshape(-1, 8, squares.shape[1]), axis=0)
        acc[...] += jnp.dot(
            wbuf[:, pl.ds(at, 2 * rows)], normed, preferred_element_type=jnp.float32
        )

    ready = [(0, 0)]
    for step, m, side in g.events():
        step(m)
        if ready:
            take(*ready.pop(0))
        ready.append((m, side))
    for item in ready:
        take(*item)

    scale = lax.rsqrt(jnp.sum(total[...], axis=0, keepdims=True) / width + EPS)
    nq = w_q.shape[0]
    nv = w_v.shape[0]
    q = (acc[0:nq] * scale).astype(jnp.bfloat16)
    k = (acc[nq : 2 * nq] * scale * DQK ** (-0.5)).astype(jnp.bfloat16)
    qk_own[0:nq] = q
    qk_own[nq : 2 * nq] = k
    mine = lax.rem(me, 8)
    copies = []

    def pass_on(mask, src, origin, slot):
        copy = pltpu.make_async_remote_copy(
            src_ref=src,
            dst_ref=qk_all.at[origin],
            send_sem=qsend.at[len(copies)],
            recv_sem=qrecv.at[slot],
            device_id=(flip(me, mask),),
            device_id_type=MESH,
        )
        copy.start()
        copies.append(copy)

    def arrived(origin, slot):
        ref = qk_all.at[origin]
        pltpu.make_async_copy(ref, ref, qrecv.at[slot]).wait()

    for mask in (6, 2, 4, 1):
        pass_on(mask, qk_own, mine, mask)
    qk_all[mine] = qk_own[...]
    kown_out[...] = k
    def column(line):
        return jnp.concatenate(
            [jnp.broadcast_to(line[:, i : i + 1], scale.shape) for i in range(heads)],
            axis=0,
        )

    gate_in = acc[row : row + heads] * scale + column(b_i)
    gate_f = acc[row + heads : row + 2 * heads] * scale + column(b_f)
    soft = jnp.minimum(gate_f, 0.0) - jnp.log1p(jnp.exp(-jnp.abs(gate_f)))
    logf = soft * (1.0 + where[...].astype(jnp.float32) / most)
    lifted = logf + maxima[...]
    new_max = jnp.maximum(lifted, gate_in)
    max_out[...] = new_max
    dec_out[...] = jnp.exp(lifted - new_max)
    fre_out[...] = jnp.exp(gate_in - new_max)
    val_out[...] = acc[2 * nq : 2 * nq + nv] * scale
    og_out[...] = jax.nn.sigmoid(acc[2 * nq + nv : 2 * nq + 2 * nv] * scale)
    for mask in (2, 4, 6):
        origin = flip(mine, mask)
        arrived(origin, mask)
        pass_on(1, qk_all.at[origin], origin, mask + 1)
    for mask in (1, 3, 5, 7):
        arrived(flip(mine, mask), mask)
    for part in range(8):
        q_out[part * nq : (part + 1) * nq] = qk_all[part, 0:nq].astype(jnp.float32)
        k_out[part * nq : (part + 1) * nq] = qk_all[part, nq : 2 * nq].astype(jnp.float32)
    for copy in copies:
        copy.wait_send()
    g.end()
    big.wait()


GROUP = 4
SLOTS = 4


def cell_kernel(
    cells, val, og, q, k, dec, fre, norms,
    new_cells, gated,
    stage, numer, fv, nrm, den, sems, nsem,
):
    me = lax.axis_index("tp")
    head = me * dec.shape[0] // lax.axis_size("tp")
    dq = q.shape[0]
    load = pltpu.make_async_copy(norms.at[pl.ds(head * dq, dq)], nrm, nsem)
    load.start()
    decay = dec[pl.ds(head, 1), :]
    fresh = fre[pl.ds(head, 1), :]
    fv[...] = fresh * val[...]
    seqs = decay.shape[1]
    decay8 = jnp.broadcast_to(decay, (8, seqs))
    number = cells.shape[0] // GROUP

    def out_copy(step, slot):
        return pltpu.make_async_copy(
            stage.at[slot], new_cells.at[pl.ds(step * GROUP, GROUP)], sems.at[slot]
        )

    def body(step, carry):
        slot = lax.rem(step, SLOTS)

        @pl.when(step >= SLOTS)
        def _():
            out_copy(step - SLOTS, slot).wait()

        lines = [
            jnp.broadcast_to(fv[pl.ds(step * GROUP + i, 1), :], (8, seqs))
            for i in range(GROUP)
        ]
        sums = [jnp.zeros((8, seqs), jnp.float32)] * GROUP
        for d in range(0, dq, 8):
            qd, kd = q[d : d + 8], k[d : d + 8]
            for i in range(GROUP):
                new = decay8 * cells[step * GROUP + i, d : d + 8] + lines[i] * kd
                stage[slot, i, d : d + 8] = new
                sums[i] = sums[i] + qd * new
        for i in range(GROUP):
            numer[pl.ds(step * GROUP + i, 1), :] = jnp.sum(
                sums[i], axis=0, keepdims=True
            )
        out_copy(step, slot).start()
        return carry

    lax.fori_loop(0, number, body, 0)
    load.wait()
    denom = jnp.sum(q[...] * (decay * nrm[...] + fresh * k[...]), axis=0, keepdims=True)
    hidden = numer[...] / jnp.maximum(jnp.abs(denom), 1.0)
    gated[...] = (hidden * og[...]).astype(jnp.bfloat16)
    for step in range(number - SLOTS, number):
        out_copy(step, step % SLOTS).wait()


def read_kernel(
    planes, gated, kown, w_read, tok, mixed, keys, gbuf, wbuf,
    send, recv, ksend, krecv, wsem,
):
    me = lax.axis_index("tp")
    load = pltpu.make_async_copy(w_read, wbuf, wsem)
    load.start()
    greet(me, plane_masks(planes))
    g = Gather(me, planes, gated, gbuf, send, recv)
    h = Gather(me, planes, kown, keys, ksend, krecv)
    g.begin()
    h.begin()
    gbuf[me] = gated[...]
    keys[me] = kown[...]
    for (step, m, _), (other, _, _) in zip(g.events(), h.events()):
        step(m)
        other(m)
    for m in range(planes):
        for side in range(4):
            g.sibling(m, side)
    load.wait()
    whole = gbuf[...].reshape(-1, gbuf.shape[2])
    out = jnp.dot(wbuf[...], whole, preferred_element_type=jnp.float32)
    mixed[...] = (tok[...].astype(jnp.float32) + out).astype(jnp.bfloat16)
    for m in range(planes):
        for side in range(4):
            h.sibling(m, side)
    g.end()
    h.end()


def fused_block(
    rows, where, gain, w_query, w_key, w_value, w_outgate, w_input, w_forget,
    bias_input, bias_forget, w_read, cells, norms, maxima,
):
    count = lax.axis_size("tp")
    planes = count // 8
    width = gain.shape[0]
    heads = w_input.shape[0]
    seqs = rows.shape[1]
    nq, nv = w_query.shape[0], w_value.shape[0]
    f32, bf16 = jnp.float32, jnp.bfloat16
    total_w = 2 * nq + 2 * nv + 16
    sends = Gather.sends(planes)
    hbm = functools.partial(
        pltpu.with_memory_space_constraint, memory_space=pltpu.HBM
    )
    dma = pltpu.SemaphoreType.DMA
    c_vm, val, og, q, k, kown, new_max, dec, fre = pl.pallas_call(
        functools.partial(project_kernel, planes, width, MOST_LEN),
        out_shape=(
            pltpu.VMEM(cells.shape, f32),
            jax.ShapeDtypeStruct((nv, seqs), f32),
            jax.ShapeDtypeStruct((nv, seqs), f32),
            jax.ShapeDtypeStruct((8 * nq, seqs), f32),
            jax.ShapeDtypeStruct((8 * nq, seqs), f32),
            jax.ShapeDtypeStruct((nq, seqs), bf16),
            jax.ShapeDtypeStruct((heads, seqs), f32),
            jax.ShapeDtypeStruct((heads, seqs), f32),
            jax.ShapeDtypeStruct((heads, seqs), f32),
        ),
        in_specs=[ANY] * 13,
        out_specs=[VM] * 9,
        scratch_shapes=[
            pltpu.VMEM((count, rows.shape[0], seqs), bf16),
            pltpu.VMEM((total_w, width), bf16),
            pltpu.VMEM((width, 128), f32),
            pltpu.VMEM((total_w, seqs), f32),
            pltpu.VMEM((8, seqs), f32),
            pltpu.VMEM((2 * nq, seqs), bf16),
            pltpu.VMEM((8, 2 * nq, seqs), bf16),
            pltpu.VMEM(rows.shape, bf16),
            pltpu.VMEM((width // 128, 128), f32),
            pltpu.VMEM(w_input.shape, bf16),
            pltpu.VMEM(w_forget.shape, bf16),
            pltpu.VMEM((1, heads), f32),
            pltpu.VMEM((1, heads), f32),
            pltpu.VMEM((1, seqs), where.dtype),
            pltpu.VMEM((heads, seqs), f32),
            dma((sends,)),
            dma((10 * planes,)),
            dma((7,)),
            dma((8,)),
            dma((4,)),
            dma,
            dma((8,)),
        ],
        compiler_params=pltpu.CompilerParams(
            collective_id=0, has_side_effects=True, vmem_limit_bytes=K1_LIMIT
        ),
        name="project",
    )(
        *map(
            hbm,
            (
                rows, gain.reshape(width // 128, 128), w_query, w_key, w_value,
                w_outgate, w_input, w_forget, bias_input[None, :],
                bias_forget[None, :], where[None, :], maxima, cells,
            ),
        )
    )
    new_cells, gated = pl.pallas_call(
        cell_kernel,
        out_shape=(
            jax.ShapeDtypeStruct(cells.shape, f32),
            jax.ShapeDtypeStruct((nv, seqs), bf16),
        ),
        in_specs=[VM] * 7 + [ANY],
        out_specs=[ANY, VM],
        scratch_shapes=[
            pltpu.VMEM((SLOTS, GROUP) + cells.shape[1:], f32),
            pltpu.VMEM((nv, seqs), f32),
            pltpu.VMEM((nv, seqs), f32),
            pltpu.VMEM((8 * nq, seqs), f32),
            pltpu.VMEM((8, seqs), f32),
            dma((SLOTS,)),
            dma,
        ],
        compiler_params=pltpu.CompilerParams(vmem_limit_bytes=K1_LIMIT),
        name="cells",
    )(
        pltpu.with_memory_space_constraint(c_vm, memory_space=pltpu.VMEM), val, og, q, k, dec, fre, norms,
    )
    mixed, keys = pl.pallas_call(
        functools.partial(read_kernel, planes),
        out_shape=(
            jax.ShapeDtypeStruct(rows.shape, bf16),
            jax.ShapeDtypeStruct((count, nq, seqs), bf16),
        ),
        in_specs=[VM, VM, ANY, VM],
        out_specs=[VM, VM],
        scratch_shapes=[
            pltpu.VMEM((count, nv, seqs), bf16),
            pltpu.VMEM(w_read.shape, bf16),
            dma((sends,)),
            dma((10 * planes,)),
            dma((sends,)),
            dma((10 * planes,)),
            dma,
        ],
        compiler_params=pltpu.CompilerParams(
            collective_id=1, has_side_effects=True, vmem_limit_bytes=K1_LIMIT
        ),
        name="readout",
    )(gated, kown, w_read, rows)
    keys = keys.astype(f32).reshape(heads, -1, seqs)
    norms_new = dec[:, None, :] * norms.reshape(keys.shape) + fre[:, None, :] * keys
    return mixed, new_cells, norms_new.reshape(norms.shape), new_max


K1_LIMIT = 30 * 1024 * 1024


def fits(count, rows, w_query, w_input, cells):
    planes = count // 8
    return (
        count % 8 == 0
        and planes & (planes - 1) == 0
        and w_input.shape[0] == planes
        and rows.shape[0] % 128 == 0
        and w_query.shape[0] % 32 == 0
        and cells.shape[0] % (GROUP * SLOTS) == 0
    )


def mix_block(
    rows,
    where,
    gain,
    w_query,
    w_key,
    w_value,
    w_outgate,
    w_input,
    w_forget,
    bias_input,
    bias_forget,
    w_read,
    cells,
    norms,
    maxima,
):
    count = lax.axis_size("tp")
    index = lax.axis_index("tp")
    seqs = rows.shape[1]
    model_width = gain.shape[0]
    heads = w_input.shape[0]
    head = index * heads // count
    whole = lax.all_gather(rows, "tp", axis=0, tiled=True).astype(jnp.float32)
    total = jnp.sum(whole * whole, axis=0)
    normed = (whole * gain[:, None]).astype(jnp.bfloat16)
    scale = lax.rsqrt(total / model_width + EPS)[None, :]
    query_loc = (jnp.dot(w_query, normed, preferred_element_type=jnp.float32) * scale).astype(
        jnp.bfloat16
    )
    key_loc = (
        jnp.dot(w_key, normed, preferred_element_type=jnp.float32) * scale * DQK ** (-0.5)
    ).astype(jnp.bfloat16)
    query_all, key_all = (
        lax.all_gather(query_loc, "tp", axis=0, tiled=True),
        lax.all_gather(key_loc, "tp", axis=0, tiled=True),
    )
    value = jnp.dot(w_value, normed, preferred_element_type=jnp.float32) * scale
    outgate = jnp.dot(w_outgate, normed, preferred_element_type=jnp.float32) * scale
    gate_in = (
        jnp.dot(w_input, normed, preferred_element_type=jnp.float32) * scale + bias_input[:, None]
    )
    gate_forget = (
        jnp.dot(w_forget, normed, preferred_element_type=jnp.float32) * scale + bias_forget[:, None]
    )
    logf = jax.nn.log_sigmoid(gate_forget) * (1.0 + where / MOST_LEN)
    new_max = jnp.maximum(logf + maxima, gate_in)
    decay = jnp.exp(logf + maxima - new_max)
    fresh = jnp.exp(gate_in - new_max)
    queries = query_all.astype(jnp.float32).reshape(heads, DQK, seqs)
    keys = key_all.astype(jnp.float32).reshape(heads, DQK, seqs)
    norms_new = decay[:, None, :] * norms.reshape(heads, DQK, seqs) + fresh[:, None, :] * keys
    denom = jnp.sum(queries * norms_new, axis=1)
    decay_own = lax.dynamic_index_in_dim(decay, head, 0)
    fresh_own = lax.dynamic_index_in_dim(fresh, head, 0)
    den_own = lax.dynamic_index_in_dim(denom, head, 0)
    q_head = lax.dynamic_slice_in_dim(query_all, head * DQK, DQK, 0).astype(jnp.float32)
    k_head = lax.dynamic_slice_in_dim(key_all, head * DQK, DQK, 0).astype(jnp.float32)
    new_cells = decay_own[None] * cells + fresh_own[None] * value[:, None, :] * k_head[None, :, :]
    numer = jnp.sum(q_head[None, :, :] * new_cells, axis=1)
    hidden = numer / jnp.maximum(jnp.abs(den_own), 1.0)
    gated = (hidden * jax.nn.sigmoid(outgate)).astype(jnp.bfloat16)
    mixed = jnp.dot(
        w_read, lax.all_gather(gated, "tp", axis=0, tiled=True), preferred_element_type=jnp.float32
    )
    new_rows = (rows.astype(jnp.float32) + mixed).astype(jnp.bfloat16)
    return (new_rows, new_cells, norms_new.reshape(heads * DQK, seqs), new_max)


def shards(
    tokens,
    positions,
    norm_gain,
    w_query,
    w_key,
    w_value,
    w_outgate,
    w_input,
    w_forget,
    bias_input,
    bias_forget,
    w_read,
    cells,
    norms,
    maxima,
):
    if fits(lax.axis_size("tp"), tokens, w_query, w_input, cells):
        block, where = fused_block, positions
    else:
        block, where = mix_block, positions.astype(jnp.float32)[None, :]
    return block(
        tokens,
        where,
        norm_gain,
        w_query,
        w_key,
        w_value,
        w_outgate,
        w_input,
        w_forget,
        bias_input,
        bias_forget,
        w_read,
        cells,
        norms,
        maxima,
    )


def solution(mesh):
    return jax.shard_map(
        shards,
        mesh=mesh,
        in_specs=(
            P("tp", None),
            P(),
            P(),
            P("tp", None),
            P("tp", None),
            P("tp", None),
            P("tp", None),
            P(),
            P(),
            P(),
            P(),
            P("tp", None),
            P("tp", None, None),
            P(),
            P(),
        ),
        out_specs=(P("tp", None), P("tp", None, None), P(), P()),
        check_vma=False,
    )
```
